32 devices in a mesh: st: 8 (over z, x), tp: 4 (over y, core).
Axes of the slice: x: 2, y: 2, z: 4, core: 2. Of those that a mesh axis runs over, the one named last changes fastest.
Arguments:
- tokens: bfloat16 [16384, 2048], P('st', 'tp'), may hold values from -48 to 48
- store: bfloat16 [256, 64, 2048], P('st'), may hold values from -48 to 48
- passage_holder_index: int32 [128, 2], P('st'), may hold values from 0 to 7, all different within a row; in each aligned block of 16 rows (0 to 15, 16 to 31, ...) at most 8 rows name the same one
- passage_slot: int32 [128, 2], P('st'), may hold values from 0 to 31
- query_weight: bfloat16 [2048, 1024], P(None, 'tp'), may hold values from -0.125 to 0.125
- key_matrix: bfloat16 [2048, 1024], P(None, 'tp'), may hold values from -0.125 to 0.125
- value_weight: bfloat16 [2048, 1024], P(None, 'tp'), may hold values from -0.125 to 0.125
- outer_gate: bfloat16 [2048, 1024], P(None, 'tp'), may hold values from -0.125 to 0.125
- inner_gate: bfloat16 [2048, 1024], P(None, 'tp'), may hold values from -0.125 to 0.125
- conv_input: bfloat16 [2048, 1024], P(None, 'tp'), may hold values from -0.125 to 0.125
- conv_taps: bfloat16 [3, 1024], P(None, 'tp'), may hold values from -3.5 to 3.5
- route_gate_projection: bfloat16 [2048, 2], replicated, may hold values from -0.125 to 0.125
- conv_out: bfloat16 [1024, 2048], P('tp'), may hold values from -0.1875 to 0.1875
- memory_out: bfloat16 [1024, 2048], P('tp'), may hold values from -0.1875 to 0.1875
Outputs:
- mixed: bfloat16 [16384, 2048], P(('st', 'tp'))
The draws below stay inside these ranges and needn't reach their ends.
Inputs may be any that keep to these rules, and one draw needn't show every extreme that they name: `passage_holder_index`: each row names 2 different owners; among the rows of one index of st (16 aligned rows) no owner is named more than 8 times, a bound that some index of st reaches.
All inputs are finite; a program needn't handle non-finite values.
Results may differ from the reference program's by a relative error of at most 0.014.
Values may be sent and summed in bfloat16 or wider, within the bound.
A program may use at most 128 MiB of HBM per device.

```python
import math
import jax
import jax.numpy as jnp
import numpy as np
from jax import lax

D = 2048
HEADS = 8
HEAD_SIZE = 128
FILTER_CHANNELS = 1024
CONV_K = 3
SEQ_LEN = 256
BLOCK = 128
NPB = 2
PLEN = 64
P_DEV = 32
MEM_WIDTH = 1024
NBLK_DEV = 16
CAP = 8
TOKENS = 16384
BLOCKS = 128
PASSAGES = 256
N_ST = 8
N_TP = 4


def draw_tokens(key, part):
    first_key = jax.random.fold_in(jax.random.fold_in(key, 11), 0)
    values = jnp.clip(jax.random.normal(first_key, (TOKENS, D), jnp.float32), -4.0, 4.0)
    return values.astype(jnp.bfloat16)


def draw_store(key, part):
    first_key = jax.random.fold_in(jax.random.fold_in(key, 23), 0)
    values = jnp.clip(jax.random.normal(first_key, (PASSAGES, PLEN, D), jnp.float32), -4.0, 4.0)
    return values.astype(jnp.bfloat16)


def set_ends(values, key, smallest, high):
    shape = values.shape
    spot = [jax.random.randint(jax.random.fold_in(key, axis), (), 0, shape[axis]) for axis in range(len(shape))]
    values = values.at[tuple(spot)].set(smallest)
    longest = shape.index(max(shape))
    spot[longest] = (spot[longest] + 1) % shape[longest]
    return values.at[tuple(spot)].set(high)


def shard_levels(key, dims, pieces, low, largest):
    level = 1.0
    for dim, shards_of in pieces:
        draws = jax.random.uniform(jax.random.fold_in(jax.random.fold_in(key, 6), dim), (shards_of,), jnp.float32, low / len(pieces), largest / len(pieces))
        level = level * jnp.repeat(jnp.exp(draws), dims[dim] // shards_of).reshape((-1,) + (1,) * (len(dims) - 1 - dim))
    return level


def rank_bounds(count, skew):
    weights = [(1 << 20) // math.isqrt(standing ** skew) + 1 for standing in range(1, count + 1)]
    scale = 1 + sum(weights) // (1 << 30)
    return np.cumsum(np.array([max(1, weight // scale) for weight in weights]))


def skewed_ids(own_key, extent, amount, skew):
    listing = rank_bounds(amount, skew)
    pick = jax.random.randint(jax.random.fold_in(own_key, 1), extent, 0, int(listing[amount - 1]))
    standing = jnp.searchsorted(jnp.asarray(listing, jnp.int32), pick, side="right")
    return jax.random.permutation(jax.random.fold_in(own_key, 2), amount)[standing].astype(jnp.int32)


def assign_block(rng, own, number, rows, count, top, limit, lean):
    sequence = jax.random.permutation(rng, count)
    heavy_load, ordinary = shares(count, rows * top, limit, lean, True), shares(count, rows * top, limit, lean, False)
    places = jnp.arange(count)

    def named(tallies, rotation):
        used = int((tallies > 0).sum())
        fixed = max(1, used // 4)
        moved = fixed + (places - fixed + rotation * (used - fixed)) % max(1, count - fixed)
        return jnp.zeros((count,), jnp.int32).at[sequence[jnp.where(places < fixed, places, moved)]].set(jnp.asarray(tallies, jnp.int32))

    tallies = jnp.where(number % 4 == 0, named(heavy_load, number // 4), named(ordinary, number - number // 4 - 1))
    mixed = jax.random.permutation(jax.random.fold_in(own, 3), count)
    donor, sink = mixed[0:count // 2 * 2:2], mixed[1:count // 2 * 2:2]
    slack = jnp.minimum(tallies[donor] - 1, limit - tallies[sink]) // 2
    slack = jnp.where((donor == sequence[0]) | (sink == sequence[0]) | (tallies[sink] == 0), 0, jnp.maximum(slack, 0))
    moved = jax.random.randint(jax.random.fold_in(own, 4), (count // 2,), 0, 1 << 20) % (slack + 1)
    tallies = tallies.at[donor].add(-moved).at[sink].add(moved)
    members = jnp.searchsorted(jnp.cumsum(tallies), jnp.arange(rows * top), side="right").astype(jnp.int32)
    listing = members.reshape(top, rows).T
    listing = listing[jax.random.permutation(jax.random.fold_in(own, 1), rows)]
    rotation = jax.random.randint(jax.random.fold_in(own, 2), (rows, 1), 0, top)
    return jnp.take_along_axis(listing, (jnp.arange(top)[None, :] + rotation) % top, axis=1)


def shares(count, total, limit, slope, full):
    loads = [(1 << 20) // math.isqrt(grade ** slope) + 1 for grade in range(1, count + 1)]
    largest = limit if full else min(limit, max(-(-total // count), total * loads[0] // sum(loads)))
    least = 1 if total - largest >= count - 1 else 0
    counts, rest = [largest] + [least] * (count - 1), total - largest - least * (count - 1)
    while rest > 0:
        candidates = [i for i in range(1, count) if counts[i] < largest] or [i for i in range(1, count) if counts[i] < limit]
        pool, budget = sum([loads[i] for i in candidates]), rest
        for i in candidates:
            more = min(limit - counts[i], max(1, budget * loads[i] // pool), rest)
            counts[i] = counts[i] + more
            rest = rest - more
    return np.array(counts)


def bell_draw(rng, dims, deviation, bound, cuts=(), held_as=jnp.bfloat16):
    entries = jax.random.normal(rng, dims, jnp.float32) * deviation
    if len(cuts) > 0:
        entries = shard_levels(rng, dims, cuts, -0.22, 0.18) * entries
    return jnp.clip(entries, min=-bound, max=bound).astype(held_as)


def setup_inputs(seed: int = 0) -> dict:
    splits = jax.random.split(jax.random.key(seed), 15)
    tokens = draw_tokens(jax.random.fold_in(splits[14], 71), 0)
    store = draw_store(jax.random.fold_in(splits[14], 71), 0)
    passage_holder_index_keys = jax.random.split(jax.random.fold_in(splits[2], 1), BLOCKS // NBLK_DEV)
    passage_holder_index_turns = jax.random.permutation(jax.random.fold_in(splits[2], 3), BLOCKS // NBLK_DEV)
    passage_holder_index = jax.vmap(lambda own, number: assign_block(jax.random.fold_in(splits[2], 2), own, number, NBLK_DEV, N_ST, NPB, CAP, 2))(passage_holder_index_keys, passage_holder_index_turns).reshape((BLOCKS, NPB))
    passage_slot = set_ends(skewed_ids(splits[3], (BLOCKS, NPB), P_DEV, 2), jax.random.fold_in(splits[3], 3), 0, P_DEV - 1).astype(jnp.int32)
    query_weight = bell_draw(splits[4], (D, MEM_WIDTH), D ** -0.5, 0.125, ((1, 4),))
    key_matrix = bell_draw(splits[5], (D, MEM_WIDTH), D ** -0.5, 0.125, ((1, 4),))
    value_weight = bell_draw(splits[6], (D, MEM_WIDTH), D ** -0.5, 0.125, ((1, 4),))
    outer_gate = bell_draw(splits[7], (D, FILTER_CHANNELS), D ** -0.5, 0.125, ((1, 4),))
    inner_gate = bell_draw(splits[8], (D, FILTER_CHANNELS), D ** -0.5, 0.125, ((1, 4),))
    conv_input = bell_draw(splits[9], (D, FILTER_CHANNELS), D ** -0.5, 0.125, ((1, 4),))
    conv_taps = bell_draw(splits[10], (CONV_K, FILTER_CHANNELS), CONV_K ** -0.5, 3.5, ((1, 4),))
    route_gate_projection = bell_draw(splits[11], (D, 2), D ** -0.5, 0.125)
    conv_out = bell_draw(splits[12], (FILTER_CHANNELS, D), FILTER_CHANNELS ** -0.5, 0.1875, ((0, 4),))
    memory_out = bell_draw(splits[13], (MEM_WIDTH, D), MEM_WIDTH ** -0.5, 0.1875, ((0, 4),))
    return {"tokens": tokens, "store": store, "passage_holder_index": passage_holder_index, "passage_slot": passage_slot, "query_weight": query_weight, "key_matrix": key_matrix, "value_weight": value_weight, "outer_gate": outer_gate, "inner_gate": inner_gate, "conv_input": conv_input, "conv_taps": conv_taps, "route_gate_projection": route_gate_projection, "conv_out": conv_out, "memory_out": memory_out}


def reference(tokens, store, passage_holder_index, passage_slot, query_weight, key_matrix, value_weight, outer_gate, inner_gate, conv_input, conv_taps, route_gate_projection, conv_out, memory_out):
    queries = jnp.dot(tokens, query_weight, preferred_element_type=jnp.float32).astype(jnp.bfloat16)
    outer_part = jnp.dot(tokens, outer_gate, preferred_element_type=jnp.float32)
    inner_part = jnp.dot(tokens, inner_gate, preferred_element_type=jnp.float32)
    value_part = jnp.dot(tokens, conv_input, preferred_element_type=jnp.float32)
    branch_mix = jax.nn.sigmoid(jnp.dot(tokens, route_gate_projection, preferred_element_type=jnp.float32))
    mixed_input = (inner_part * value_part).reshape(TOKENS // SEQ_LEN, SEQ_LEN, FILTER_CHANNELS)
    padded_input = jnp.pad(mixed_input, ((0, 0), (CONV_K - 1, 0), (0, 0)))
    tap_values = conv_taps.astype(jnp.float32)
    filtered_signal = tap_values[0] * padded_input[:, 0:SEQ_LEN]
    for offset in range(1, CONV_K):
        filtered_signal = filtered_signal + tap_values[offset] * padded_input[:, offset:offset + SEQ_LEN]
    conv_branch = (outer_part * filtered_signal.reshape(TOKENS, FILTER_CHANNELS)).astype(jnp.bfloat16)

    passage_ids = (passage_holder_index * P_DEV + passage_slot).reshape(-1).astype(jnp.int32)
    memory_rows = store[passage_ids].reshape(-1, D)
    passage_key_rows = jnp.dot(memory_rows, key_matrix, preferred_element_type=jnp.float32).astype(jnp.bfloat16)
    retrieved_content_vectors = jnp.dot(memory_rows, value_weight, preferred_element_type=jnp.float32).astype(jnp.bfloat16)
    passage_key_rows = passage_key_rows.reshape(BLOCKS, NPB * PLEN, HEADS, HEAD_SIZE)
    retrieved_content_vectors = retrieved_content_vectors.reshape(BLOCKS, NPB * PLEN, HEADS, HEAD_SIZE)
    query_block_rows = queries.reshape(BLOCKS, BLOCK, HEADS, HEAD_SIZE)
    scores = jnp.einsum('bqhd,bkhd->bhqk', query_block_rows.astype(jnp.float32), passage_key_rows.astype(jnp.float32)) * (HEAD_SIZE ** -0.5)
    softmax_shares = jax.nn.softmax(scores, axis=-1).astype(jnp.bfloat16)
    memory_branch = jnp.einsum('bhqk,bkhd->bqhd', softmax_shares.astype(jnp.float32), retrieved_content_vectors.astype(jnp.float32))
    memory_branch = memory_branch.reshape(TOKENS, MEM_WIDTH).astype(jnp.bfloat16)

    conv_cols = FILTER_CHANNELS // N_TP
    head_cols = MEM_WIDTH // N_TP
    summed = jnp.zeros((TOKENS, D), jnp.float32)
    for tensor_parallel_team in range(N_TP):
        conv_slice = conv_branch[:, tensor_parallel_team * conv_cols:(tensor_parallel_team + 1) * conv_cols]
        memory_slice = memory_branch[:, tensor_parallel_team * head_cols:(tensor_parallel_team + 1) * head_cols]
        share_term = (branch_mix[:, 0:1] * jnp.dot(conv_slice, conv_out[tensor_parallel_team * conv_cols:(tensor_parallel_team + 1) * conv_cols], preferred_element_type=jnp.float32)
                      + branch_mix[:, 1:2] * jnp.dot(memory_slice, memory_out[tensor_parallel_team * head_cols:(tensor_parallel_team + 1) * head_cols], preferred_element_type=jnp.float32))
        summed = summed + lax.optimization_barrier(share_term.astype(jnp.bfloat16)).astype(jnp.float32)
    return summed.astype(jnp.bfloat16)
```

```python
import functools

import jax
import jax.numpy as jnp
from jax import lax
from jax.experimental import pallas as pl
from jax.experimental.pallas import tpu as pltpu
from jax.sharding import PartitionSpec as P

HEAD_SIZE = 128
CONV_K = 3
SEQ_LEN = 256
BLOCK = 128
NPB = 2
PLEN = 64
CORES = 2


def attention_kernel(group, target_ref, q_ref, table_ref, out_ref):
    first = pl.program_id(0) * group
    for i in range(group):
        rows = slice(i * BLOCK, (i + 1) * BLOCK)
        pieces = [table_ref[target_ref[(first + i) * NPB + j]] for j in range(NPB)]
        joined = jnp.concatenate(pieces, axis=0)
        keys, values = joined[:, :HEAD_SIZE], joined[:, HEAD_SIZE:]
        scores = lax.dot_general(
            q_ref[rows, :], keys, (((1,), (1,)), ((), ())), preferred_element_type=jnp.float32
        ) * HEAD_SIZE ** (-0.5)
        scores = jnp.exp(scores - jnp.max(scores, axis=1, keepdims=True))
        weights = (scores / jnp.sum(scores, axis=1, keepdims=True)).astype(jnp.bfloat16)
        out_ref[rows, :] = jnp.dot(weights, values, preferred_element_type=jnp.float32).astype(
            jnp.bfloat16
        )


def attention(queries, head, table, target):
    row_count = queries.shape[0]
    block_count = row_count // BLOCK
    group = 4
    while block_count % group:
        group //= 2
    return pl.pallas_call(
        functools.partial(attention_kernel, group),
        out_shape=jax.ShapeDtypeStruct((row_count, HEAD_SIZE), jnp.bfloat16),
        grid_spec=pltpu.PrefetchScalarGridSpec(
            num_scalar_prefetch=1,
            grid=(block_count // group,),
            in_specs=[
                pl.BlockSpec((group * BLOCK, HEAD_SIZE), lambda i, t: (i, head)),
                pl.BlockSpec(table.shape, lambda i, t: (0, 0, 0)),
            ],
            out_specs=pl.BlockSpec((group * BLOCK, HEAD_SIZE), lambda i, t: (i, 0)),
        ),
        compiler_params=pltpu.CompilerParams(vmem_limit_bytes=24 * 1024 * 1024),
        cost_estimate=pl.CostEstimate(
            flops=4 * row_count * NPB * PLEN * HEAD_SIZE,
            bytes_accessed=2 * table.size + 4 * row_count * HEAD_SIZE,
            transcendentals=row_count * NPB * PLEN,
        ),
    )(target, queries, table)


def local(
    tokens,
    store,
    passage_holder_index,
    passage_slot,
    query_weight,
    key_matrix,
    value_weight,
    outer_gate,
    inner_gate,
    conv_input,
    conv_taps,
    route_gate_projection,
    conv_out,
    memory_out,
):
    row_count, features = tokens.shape
    head_width = query_weight.shape[1]
    local_heads = head_width // HEAD_SIZE
    conv_cols = outer_gate.shape[1]
    team = lax.axis_size("tp")
    chips = team // CORES
    me = lax.axis_index("tp")
    my_chip, my_core = me // CORES, me % CORES
    chip_rows = row_count // chips
    own_rows = row_count // team

    def shift(value, step):
        pairs = [(i, (i + CORES * step) % team) for i in range(team)]
        return lax.ppermute(value, "tp", pairs)

    def swap(value):
        pairs = [(i, i - i % CORES + (CORES - 1 - i % CORES)) for i in range(team)]
        return lax.ppermute(value, "tp", pairs)

    owners = passage_holder_index.reshape(-1)
    local_slots = passage_slot.reshape(-1)
    owner_count = lax.axis_size("st")
    request_count = owners.shape[0]
    capacity = max(2, 2 * request_count // owner_count)
    one_hot = (owners[:, None] == jnp.arange(owner_count, dtype=jnp.int32)[None, :]).astype(
        jnp.int32
    )
    before = jnp.cumsum(one_hot, axis=0) - one_hot
    position = jnp.sum(before * one_hot, axis=1)
    target = owners * capacity + position
    matches = (
        target[:, None] == jnp.arange(owner_count * capacity, dtype=jnp.int32)[None, :]
    ).astype(jnp.int32)
    outgoing = jnp.sum(matches * local_slots[:, None], axis=0).reshape(owner_count, capacity)
    wanted = lax.all_to_all(outgoing, "st", split_axis=0, concat_axis=0, tiled=True)

    own_columns = [tokens] + [shift(tokens, k) for k in range(1, chips)]
    near = swap(tokens)
    far = [swap(piece) for piece in own_columns[1:]]
    pieces = jnp.concatenate(own_columns + [near] + far, axis=1)
    order = jnp.stack(
        [
            ((my_chip + chips - k) % chips) * CORES + core
            for core in (my_core, CORES - 1 - my_core)
            for k in range(chips)
        ]
    )

    flat_rows = store.reshape(-1, store.shape[-1])
    served = []
    for head in range(local_heads):
        columns = slice(head * HEAD_SIZE, (head + 1) * HEAD_SIZE)
        weight = jnp.concatenate([key_matrix[:, columns], value_weight[:, columns]], axis=1)
        table = jnp.dot(flat_rows, weight, preferred_element_type=jnp.float32).astype(jnp.bfloat16)
        table = table.reshape(store.shape[:-1] + (2 * HEAD_SIZE,))
        chosen = table[wanted.reshape(-1)].reshape(wanted.shape + table.shape[1:])
        arrived = lax.all_to_all(chosen, "st", split_axis=0, concat_axis=0, tiled=True)
        served.append(arrived.reshape(owner_count * capacity, PLEN, 2 * HEAD_SIZE))

    out_weights = jnp.stack([conv_out, memory_out])
    if chips > 1:
        out_weights, _ = lax.optimization_barrier((out_weights, own_columns[-1]))
    own_weights = [out_weights] + [shift(out_weights, k) for k in range(1, chips)]
    all_weights = jnp.concatenate(
        own_weights + [swap(piece) for piece in own_weights], axis=1
    )

    local_weight = jnp.concatenate([query_weight, outer_gate, inner_gate, conv_input], axis=1)
    local_weight = local_weight.reshape(team, features, -1)[order].reshape(team * features, -1)
    gate_weight = route_gate_projection.reshape(team, features, -1)[order]
    gate_weight = gate_weight.reshape(team * features, -1)
    projected = jnp.dot(pieces, local_weight, preferred_element_type=jnp.float32)
    queries = projected[:, :head_width].astype(jnp.bfloat16)
    outer_part = projected[:, head_width : head_width + conv_cols]
    inner_part = projected[:, head_width + conv_cols : head_width + 2 * conv_cols]
    value_part = projected[:, head_width + 2 * conv_cols :]
    own_pieces = lax.dynamic_slice_in_dim(pieces, me * own_rows, own_rows, 0)
    branch_mix = jax.nn.sigmoid(
        jnp.dot(own_pieces, gate_weight, preferred_element_type=jnp.float32)
    )
    seq_count = row_count // SEQ_LEN
    mixed_input = (inner_part * value_part).reshape(seq_count, SEQ_LEN, conv_cols)
    padded_input = jnp.pad(mixed_input, ((0, 0), (CONV_K - 1, 0), (0, 0)))
    tap_values = conv_taps.astype(jnp.float32)
    filtered_signal = tap_values[0] * padded_input[:, 0:SEQ_LEN]
    for offset in range(1, CONV_K):
        filtered_signal = (
            filtered_signal + tap_values[offset] * padded_input[:, offset : offset + SEQ_LEN]
        )
    conv_branch = (outer_part * filtered_signal.reshape(row_count, conv_cols)).astype(jnp.bfloat16)

    def to_rows(branch):
        parts = []
        for k in range(chips):
            start = ((my_chip + k) % chips) * chip_rows
            part = lax.dynamic_slice_in_dim(branch, start, chip_rows, 0)
            parts.append(part if k == 0 else shift(part, k))
        kept, given = [], []
        for part in parts:
            kept.append(lax.dynamic_slice_in_dim(part, my_core * own_rows, own_rows, 0))
            other = lax.dynamic_slice_in_dim(part, (CORES - 1 - my_core) * own_rows, own_rows, 0)
            given.append(swap(other))
        return kept + given

    conv_rows = jnp.concatenate(to_rows(conv_branch), axis=1)
    conv_sum = jnp.dot(conv_rows, all_weights[0], preferred_element_type=jnp.float32)
    total = branch_mix[:, 0:1] * conv_sum

    per_head = [
        to_rows(attention(queries, head, served[head], target)) for head in range(local_heads)
    ]
    memory_rows = jnp.concatenate(
        [per_head[head][j] for j in range(team) for head in range(local_heads)], axis=1
    )
    memory_sum = jnp.dot(memory_rows, all_weights[1], preferred_element_type=jnp.float32)
    return (total + branch_mix[:, 1:2] * memory_sum).astype(jnp.bfloat16)


def solution(mesh):
    return jax.shard_map(
        local,
        mesh=mesh,
        in_specs=(
            P("st", "tp"),
            P("st", None, None),
            P("st", None),
            P("st", None),
            P(None, "tp"),
            P(None, "tp"),
            P(None, "tp"),
            P(None, "tp"),
            P(None, "tp"),
            P(None, "tp"),
            P(None, "tp"),
            P(),
            P("tp", None),
            P("tp", None),
        ),
        out_specs=P(("st", "tp"), None),
        check_vma=False,
    )
```

```python
import functools

import jax
import jax.numpy as jnp
from jax import lax
from jax.experimental import pallas as pl
from jax.experimental.pallas import tpu as pltpu
from jax.sharding import PartitionSpec as P


HEAD_SIZE = 128
CONV_K = 3
SEQ_LEN = 256
BLOCK = 128
NPB = 2
PLEN = 64
CORES = 2


def projection_kernel(x_ref, key_ref, value_ref, out_ref):
    rows = x_ref[...]
    keys = jnp.dot(rows, key_ref[...], preferred_element_type=jnp.float32).astype(jnp.bfloat16)
    values = jnp.dot(rows, value_ref[...], preferred_element_type=jnp.float32).astype(jnp.bfloat16)
    for start in range(0, keys.shape[1], HEAD_SIZE):
        middle, end = 2 * start + HEAD_SIZE, 2 * start + 2 * HEAD_SIZE
        out_ref[:, 2 * start : middle] = keys[:, start : start + HEAD_SIZE]
        out_ref[:, middle:end] = values[:, start : start + HEAD_SIZE]


def project_passages(flat_rows, key_matrix, value_weight):
    count, depth = flat_rows.shape
    width = key_matrix.shape[1]
    tile = 256
    while count % tile:
        tile //= 2
    return pl.pallas_call(
        projection_kernel,
        out_shape=jax.ShapeDtypeStruct((count, 2 * width), jnp.bfloat16),
        grid=(count // tile,),
        in_specs=[
            pl.BlockSpec((tile, depth), lambda i: (i, 0)),
            pl.BlockSpec((depth, width), lambda i: (0, 0)),
            pl.BlockSpec((depth, width), lambda i: (0, 0)),
        ],
        out_specs=pl.BlockSpec((tile, 2 * width), lambda i: (i, 0)),
        compiler_params=pltpu.CompilerParams(vmem_limit_bytes=56 * 1024 * 1024),
        cost_estimate=pl.CostEstimate(
            flops=4 * count * depth * width,
            bytes_accessed=2 * (count * depth + 2 * depth * width + 2 * count * width),
            transcendentals=0,
        ),
    )(flat_rows, key_matrix, value_weight)


def output_kernel(parts, total_ref, gate_ref, weight_ref, *refs):
    rows = jnp.concatenate([refs[i][...] for i in range(parts)], axis=1)
    product = jnp.dot(rows, weight_ref[...], preferred_element_type=jnp.float32)
    refs[parts][...] = (total_ref[...] + gate_ref[:, 1:2] * product).astype(jnp.bfloat16)


def output_rows(total, gates, weights, pieces):
    count, width = total.shape
    depth = weights.shape[0]
    tile = 512
    while width % tile:
        tile //= 2
    return pl.pallas_call(
        functools.partial(output_kernel, len(pieces)),
        out_shape=jax.ShapeDtypeStruct((count, width), jnp.bfloat16),
        grid=(width // tile,),
        in_specs=[
            pl.BlockSpec((count, tile), lambda i: (0, i)),
            pl.BlockSpec(gates.shape, lambda i: (0, 0)),
            pl.BlockSpec((depth, tile), lambda i: (0, i)),
        ]
        + [pl.BlockSpec(piece.shape, lambda i: (0, 0)) for piece in pieces],
        out_specs=pl.BlockSpec((count, tile), lambda i: (0, i)),
        compiler_params=pltpu.CompilerParams(vmem_limit_bytes=32 * 1024 * 1024),
        cost_estimate=pl.CostEstimate(
            flops=2 * count * depth * width,
            bytes_accessed=6 * count * width + 2 * depth * width + 2 * count * depth,
            transcendentals=0,
        ),
    )(total, gates, weights, *pieces)


def attention_kernel(group, target_ref, q_ref, table_ref, out_ref):
    first = pl.program_id(0) * group
    joined, weights = [], []
    for i in range(group):
        pieces = [table_ref[target_ref[(first + i) * NPB + j]] for j in range(NPB)]
        joined.append(jnp.concatenate(pieces, axis=0))
        scores = lax.dot_general(
            q_ref[i * BLOCK : (i + 1) * BLOCK, :],
            joined[i][:, :HEAD_SIZE],
            (((1,), (1,)), ((), ())),
            preferred_element_type=jnp.float32,
        ) * HEAD_SIZE ** (-0.5)
        scores = jnp.exp(scores - jnp.max(scores, axis=1, keepdims=True))
        weights.append((scores / jnp.sum(scores, axis=1, keepdims=True)).astype(jnp.bfloat16))
    for i in range(group):
        out_ref[i * BLOCK : (i + 1) * BLOCK, :] = jnp.dot(
            weights[i], joined[i][:, HEAD_SIZE:], preferred_element_type=jnp.float32
        ).astype(jnp.bfloat16)


def attention(queries, head, table, target):
    row_count = queries.shape[0]
    block_count = row_count // BLOCK
    group = 8
    while block_count % group:
        group //= 2
    return pl.pallas_call(
        functools.partial(attention_kernel, group),
        out_shape=jax.ShapeDtypeStruct((row_count, HEAD_SIZE), jnp.bfloat16),
        grid_spec=pltpu.PrefetchScalarGridSpec(
            num_scalar_prefetch=1,
            grid=(block_count // group,),
            in_specs=[
                pl.BlockSpec((group * BLOCK, HEAD_SIZE), lambda i, t: (i, head)),
                pl.BlockSpec(table.shape[:2] + (2 * HEAD_SIZE,), lambda i, t: (0, 0, head)),
            ],
            out_specs=pl.BlockSpec((group * BLOCK, HEAD_SIZE), lambda i, t: (i, 0)),
        ),
        compiler_params=pltpu.CompilerParams(vmem_limit_bytes=44 * 1024 * 1024),
        cost_estimate=pl.CostEstimate(
            flops=4 * row_count * NPB * PLEN * HEAD_SIZE,
            bytes_accessed=4 * HEAD_SIZE * table.shape[0] * PLEN + 4 * row_count * HEAD_SIZE,
            transcendentals=row_count * NPB * PLEN,
        ),
    )(target, queries, table)


def local(
    tokens,
    store,
    passage_holder_index,
    passage_slot,
    query_weight,
    key_matrix,
    value_weight,
    outer_gate,
    inner_gate,
    conv_input,
    conv_taps,
    route_gate_projection,
    conv_out,
    memory_out,
):
    row_count, features = tokens.shape
    head_width = query_weight.shape[1]
    local_heads = head_width // HEAD_SIZE
    conv_cols = outer_gate.shape[1]
    team = lax.axis_size("tp")
    chips = team // CORES
    me = lax.axis_index("tp")
    my_chip, my_core = me // CORES, me % CORES
    own_rows = row_count // team

    def send(value, step, other_core):
        pairs = []
        for i in range(team):
            core = CORES - 1 - i % CORES if other_core else i % CORES
            pairs.append((i, (i // CORES + step) % chips * CORES + core))
        return lax.ppermute(value, "tp", pairs)

    def shift(value, step):
        return send(value, step, False)

    def swap(value):
        return send(value, 0, True)

    owners = passage_holder_index.reshape(-1)
    local_slots = passage_slot.reshape(-1)
    owner_count = lax.axis_size("st")
    request_count = owners.shape[0]
    capacity = max(2, 2 * request_count // owner_count)
    one_hot = (owners[:, None] == jnp.arange(owner_count, dtype=jnp.int32)[None, :]).astype(
        jnp.int32
    )
    before = jnp.cumsum(one_hot, axis=0) - one_hot
    position = jnp.sum(before * one_hot, axis=1)
    target = owners * capacity + position
    matches = (
        target[:, None] == jnp.arange(owner_count * capacity, dtype=jnp.int32)[None, :]
    ).astype(jnp.int32)
    outgoing = jnp.sum(matches * local_slots[:, None], axis=0).reshape(owner_count, capacity)
    wanted = lax.all_to_all(outgoing, "st", split_axis=0, concat_axis=0, tiled=True)

    own_columns = [tokens] + [shift(tokens, k) for k in range(1, chips)]
    near = swap(tokens)
    far = [swap(piece) for piece in own_columns[1:]]
    pieces = jnp.concatenate(own_columns + [near] + far, axis=1)
    order = jnp.stack(
        [
            ((my_chip + chips - k) % chips) * CORES + core
            for core in (my_core, CORES - 1 - my_core)
            for k in range(chips)
        ]
    )

    flat_rows = store.reshape(-1, store.shape[-1])
    table = project_passages(flat_rows, key_matrix, value_weight)
    table = table.reshape(store.shape[:-1] + (2 * head_width,))
    chosen = table[wanted.reshape(-1)].reshape(wanted.shape + table.shape[1:])
    served = lax.all_to_all(chosen, "st", split_axis=0, concat_axis=0, tiled=True)
    served = served.reshape(owner_count * capacity, PLEN, 2 * head_width)

    out_weights = jnp.stack([conv_out, memory_out])
    own_weights = [out_weights] + [shift(out_weights, k) for k in range(1, chips)]
    near_weights = swap(out_weights)
    far_weights = [swap(piece) for piece in own_weights[1:]]
    all_weights = own_weights + [near_weights] + far_weights
    conv_weight = jnp.concatenate([piece[0] for piece in all_weights], axis=0)
    memory_weight = jnp.concatenate([piece[1] for piece in all_weights], axis=0)

    local_weight = jnp.concatenate([query_weight, outer_gate, inner_gate, conv_input], axis=1)
    local_weight = local_weight.reshape(team, features, -1)[order].reshape(team * features, -1)
    gate_weight = route_gate_projection.reshape(team, features, -1)[order]
    gate_weight = gate_weight.reshape(team * features, -1)
    projected = jnp.dot(pieces, local_weight, preferred_element_type=jnp.float32)
    queries = projected[:, :head_width].astype(jnp.bfloat16)
    outer_part = projected[:, head_width : head_width + conv_cols]
    inner_part = projected[:, head_width + conv_cols : head_width + 2 * conv_cols]
    value_part = projected[:, head_width + 2 * conv_cols :]
    own_pieces = lax.dynamic_slice_in_dim(pieces, me * own_rows, own_rows, 0)
    branch_mix = jax.nn.sigmoid(
        jnp.dot(own_pieces, gate_weight, preferred_element_type=jnp.float32)
    )
    seq_count = row_count // SEQ_LEN
    mixed_input = (inner_part * value_part).reshape(seq_count, SEQ_LEN, conv_cols)
    padded_input = jnp.pad(mixed_input, ((0, 0), (CONV_K - 1, 0), (0, 0)))
    tap_values = conv_taps.astype(jnp.float32)
    filtered_signal = tap_values[0] * padded_input[:, 0:SEQ_LEN]
    for offset in range(1, CONV_K):
        filtered_signal = (
            filtered_signal + tap_values[offset] * padded_input[:, offset : offset + SEQ_LEN]
        )
    conv_branch = (outer_part * filtered_signal.reshape(row_count, conv_cols)).astype(jnp.bfloat16)

    def to_rows(branch):
        parts = []
        for other_core in (False, True):
            for k in range(chips):
                core = CORES - 1 - my_core if other_core else my_core
                owner = (my_chip + k) % chips * CORES + core
                part = lax.dynamic_slice_in_dim(branch, owner * own_rows, own_rows, 0)
                parts.append(send(part, k, other_core) if k or other_core else part)
        return parts

    conv_rows = jnp.concatenate(to_rows(conv_branch), axis=1)
    conv_sum = jnp.dot(conv_rows, conv_weight, preferred_element_type=jnp.float32)
    total = branch_mix[:, 0:1] * conv_sum

    served, total, memory_weight = lax.optimization_barrier((served, total, memory_weight))
    per_head = [to_rows(attention(queries, head, served, target)) for head in range(local_heads)]
    memory_parts = [per_head[head][j] for j in range(team) for head in range(local_heads)]
    return output_rows(total, branch_mix, memory_weight, memory_parts)


def solution(mesh):
    return jax.shard_map(
        local,
        mesh=mesh,
        in_specs=(
            P("st", "tp"),
            P("st", None, None),
            P("st", None),
            P("st", None),
            P(None, "tp"),
            P(None, "tp"),
            P(None, "tp"),
            P(None, "tp"),
            P(None, "tp"),
            P(None, "tp"),
            P(None, "tp"),
            P(),
            P("tp", None),
            P("tp", None),
        ),
        out_specs=P(("st", "tp"), None),
        check_vma=False,
    )
```
